32 devices in a mesh: tp: 8 (over z, core), dp: 4 (over y, x).
Axes of the slice: x: 2, y: 2, z: 4, core: 2. Of those that a mesh axis runs over, the one named last changes fastest.
Arguments:
- tokens: bfloat16 [32, 4096], P('tp', 'dp'), may hold values from -6 to 6
- norm_gain: bfloat16 [2, 4096], P(None, 'dp'), may hold values from 0.099609375 to 1.8984375
- w_query: bfloat16 [2, 4096, 1024], P(None, 'dp', 'tp'), may hold values from -0.09375 to 0.09375
- w_key: bfloat16 [2, 4096, 1024], P(None, 'dp', 'tp'), may hold values from -0.09375 to 0.09375
- w_value: bfloat16 [2, 4096, 1024], P(None, 'dp', 'tp'), may hold values from -0.09375 to 0.09375
- w_outgate: bfloat16 [2, 4096, 1024], P(None, 'dp', 'tp'), may hold values from -0.09375 to 0.09375
- w_gates: bfloat16 [2, 4096, 16], P(None, 'dp'), may hold values from -0.09375 to 0.09375
- gate_bias: float32 [2, 2, 8], P(None, None, 'tp'), may hold values from -1 to 5
- w_out: bfloat16 [2, 1024, 4096], P(None, 'tp', 'dp'), may hold values from -0.1875 to 0.1875
- memory: float32 [2, 32, 8, 128, 128], P(None, 'dp', 'tp'), may hold values from -6 to 6
- normalizer: float32 [2, 32, 8, 128], P(None, 'dp', 'tp'), may hold values from -3 to 3
- stabilizer: float32 [2, 32, 8], P(None, 'dp', 'tp'), may hold values from -8 to 300, as said below
Outputs:
- mixed: bfloat16 [32, 4096], P('tp', 'dp')
- new_memory: float32 [2, 32, 8, 128, 128], P(None, 'dp', 'tp')
- new_normalizer: float32 [2, 32, 8, 128], P(None, 'dp', 'tp')
- new_stabilizer: float32 [2, 32, 8], P(None, 'dp', 'tp')
The draws below stay inside these ranges and needn't reach their ends.
Inputs may be any that keep to these rules, and one draw needn't show every extreme that they name: `stabilizer`: lies between -8 and 8, except that some entries may be as large as 300.
All inputs are finite; a program needn't handle non-finite values.
Results may differ from the reference program's by a relative error of at most 0.04.
Values may be sent and summed in bfloat16 or wider, within the bound.
No kernel may reach another device: no remote copies, remote signals or barrier semaphores. Data moves between devices by JAX's collectives and lax.ppermute only.
A program may use at most 64 MiB of HBM per device.

```python
import jax
import jax.numpy as jnp
from jax import lax

D = 4096
HEAD_SIZE = 128
HEADS = 8
SEQS = 32


def draw_stabilizer(key, part):
    shape = (2, SEQS, HEADS)
    values = jnp.clip(2.0 * jax.random.normal(jax.random.fold_in(key, 11), shape, jnp.float32), -8.0, 8.0)
    return values


def shard_levels(own_key, dims, shards, least, high):
    factor_of, own = 1.0, jax.random.fold_in(own_key, 6)
    for dim, shards_of in shards:
        draws = jnp.exp(jax.random.uniform(jax.random.fold_in(own, dim), (shards_of,), jnp.float32, least / len(shards), high / len(shards)))
        factor_of = factor_of * jnp.repeat(draws, dims[dim] // shards_of).reshape([-1 if axis == dim else 1 for axis in range(len(dims))])
    return factor_of


def scatter_about(key, dims, deviation, most, shards=(), held_as=jnp.bfloat16):
    drawn = jax.random.normal(key, dims, jnp.float32) * deviation
    if len(shards) > 0:
        drawn = shard_levels(key, dims, shards, -0.22, 0.18) * drawn
    return jnp.clip(drawn, min=-most, max=most).astype(held_as)


def setup_inputs(seed: int = 0) -> dict:
    splits = jax.random.split(jax.random.key(seed), 13)
    return {
        "tokens": scatter_about(splits[0], (SEQS, D), 1.0, 6.0, ((0, 8), (1, 4))),
        "norm_gain": jnp.clip(1.0 + 0.18 * jax.random.normal(splits[1], (2, D), jnp.float32), 0.099609375, 1.8984375).astype(jnp.bfloat16),
        "w_query": scatter_about(splits[2], (2, D, HEADS * HEAD_SIZE), D ** -0.5, 0.09375, ((1, 4), (2, 8))),
        "w_key": scatter_about(splits[3], (2, D, HEADS * HEAD_SIZE), D ** -0.5, 0.09375, ((1, 4), (2, 8))),
        "w_value": scatter_about(splits[4], (2, D, HEADS * HEAD_SIZE), D ** -0.5, 0.09375, ((1, 4), (2, 8))),
        "w_outgate": scatter_about(splits[5], (2, D, HEADS * HEAD_SIZE), D ** -0.5, 0.09375, ((1, 4), (2, 8))),
        "w_gates": scatter_about(splits[6], (2, D, 2 * HEADS), D ** -0.5, 0.09375, ((1, 4),)),
        "gate_bias": jnp.clip(-1.0 + 6.0 * jax.random.uniform(splits[7], (2, 2, HEADS), jnp.float32) ** shard_levels(splits[7], (2, 2, HEADS), ((2, 8),), -0.2, 0.2), -1.0, 5.0),
        "w_out": scatter_about(splits[8], (2, HEADS * HEAD_SIZE, D), (HEADS * HEAD_SIZE) ** -0.5, 0.1875, ((1, 8), (2, 4))),
        "memory": scatter_about(splits[9], (2, SEQS, HEADS, HEAD_SIZE, HEAD_SIZE), 1.0, 6.0, ((1, 4), (2, 8)), jnp.float32),
        "normalizer": scatter_about(splits[10], (2, SEQS, HEADS, HEAD_SIZE), 0.5, 3.0, ((1, 4), (2, 8)), jnp.float32),
        "stabilizer": draw_stabilizer(jax.random.fold_in(splits[12], 71), 0),
    }


epsilon = 1e-06

def cell_update(query, key_rows, value_rows, input_pre, forget_pre, memory, normalizer, stabilizer):
    batch_size = query.shape[0]
    head_count = input_pre.shape[1]
    query_float = query.astype(jnp.float32).reshape(batch_size, head_count, -1)
    key_float = key_rows.astype(jnp.float32).reshape(batch_size, head_count, -1) * query_float.shape[2] ** (-0.5)
    value_float = value_rows.astype(jnp.float32).reshape(batch_size, head_count, -1)
    carried = jax.nn.log_sigmoid(forget_pre) + stabilizer
    new_max = jnp.maximum(carried, input_pre)
    keep_factor = jnp.exp(carried - new_max)
    write_factor = jnp.exp(input_pre - new_max)
    new_memory = keep_factor[:, :, None, None] * memory + write_factor[:, :, None, None] * value_float[:, :, :, None] * key_float[:, :, None, :]
    new_normalizer = keep_factor[:, :, None] * normalizer + write_factor[:, :, None] * key_float
    numerator = lax.optimization_barrier(jnp.sum(new_memory * query_float[:, :, None, :], axis=3))
    denominator = lax.optimization_barrier(jnp.sum(new_normalizer * query_float, axis=2))
    floor_value = jnp.maximum(jnp.abs(denominator), jnp.exp(-new_max))
    readout = numerator / jnp.maximum(floor_value, 1.0)[:, :, None]
    return (readout.reshape(batch_size, -1), new_memory, new_normalizer, new_max)

def reference(tokens, norm_gain, w_query, w_key, w_value, w_outgate, w_gates, gate_bias, w_out, memory, normalizer, stabilizer):
    current = tokens
    memories = []
    normalizers = []
    maxima = []
    for layer_index in range(2):
        wide_rows = current.astype(jnp.float32)
        inv_scale = lax.rsqrt(lax.optimization_barrier(jnp.sum(wide_rows * wide_rows, axis=1)) / D + epsilon)[:, None]
        scaled = (wide_rows * norm_gain[layer_index].astype(jnp.float32)[None, :]).astype(jnp.bfloat16)
        query = (jnp.dot(scaled, w_query[layer_index], preferred_element_type=jnp.float32) * inv_scale).astype(jnp.bfloat16)
        key_rows = (jnp.dot(scaled, w_key[layer_index], preferred_element_type=jnp.float32) * inv_scale).astype(jnp.bfloat16)
        value_rows = (jnp.dot(scaled, w_value[layer_index], preferred_element_type=jnp.float32) * inv_scale).astype(jnp.bfloat16)
        outgate = (jnp.dot(scaled, w_outgate[layer_index], preferred_element_type=jnp.float32) * inv_scale).astype(jnp.bfloat16)
        gate_pre = jnp.dot(scaled, w_gates[layer_index], preferred_element_type=jnp.float32) * inv_scale
        input_pre = gate_pre[:, :HEADS] + gate_bias[layer_index, 0][None, :]
        forget_pre = gate_pre[:, HEADS:] + gate_bias[layer_index, 1][None, :]
        readout, new_memory, new_normalizer, new_max = cell_update(query, key_rows, value_rows, input_pre, forget_pre, memory[layer_index], normalizer[layer_index], stabilizer[layer_index])
        gated = (jax.nn.sigmoid(outgate.astype(jnp.float32)) * readout).astype(jnp.bfloat16)
        projected = jnp.dot(gated, w_out[layer_index], preferred_element_type=jnp.float32)
        current = (wide_rows + projected).astype(jnp.bfloat16)
        memories.append(new_memory)
        normalizers.append(new_normalizer)
        maxima.append(new_max)
    return (current, jnp.stack(memories), jnp.stack(normalizers), jnp.stack(maxima))
```

```python
import jax
import jax.numpy as jnp
from jax import lax
from jax.sharding import PartitionSpec as P

D = 4096
HEAD_SIZE = 128


epsilon = 1e-06


def cell_update(query, key_rows, value_rows, input_pre, forget_pre, memory, normalizer, stabilizer):
    batch_size = query.shape[0]
    head_count = input_pre.shape[1]
    query_float = query.astype(jnp.float32).reshape(batch_size, head_count, -1)
    key_float = key_rows.astype(jnp.float32).reshape(
        batch_size, head_count, -1
    ) * query_float.shape[2] ** (-0.5)
    value_float = value_rows.astype(jnp.float32).reshape(batch_size, head_count, -1)
    carried = jax.nn.log_sigmoid(forget_pre) + stabilizer
    new_max = jnp.maximum(carried, input_pre)
    keep_factor = jnp.exp(carried - new_max)
    write_factor = jnp.exp(input_pre - new_max)
    new_memory = (
        keep_factor[:, :, None, None] * memory
        + write_factor[:, :, None, None] * value_float[:, :, :, None] * key_float[:, :, None, :]
    )
    new_normalizer = keep_factor[:, :, None] * normalizer + write_factor[:, :, None] * key_float
    numerator = jnp.sum(new_memory * query_float[:, :, None, :], axis=3)
    denominator = jnp.sum(new_normalizer * query_float, axis=2)
    floor_value = jnp.maximum(jnp.abs(denominator), jnp.exp(-new_max))
    readout = numerator / jnp.maximum(floor_value, 1.0)[:, :, None]
    return (readout.reshape(batch_size, -1), new_memory, new_normalizer, new_max)


def peers(axis):
    size = lax.axis_size(axis)
    return size, lax.axis_index(axis)


def gather_direct(rows, axis):
    size, own = peers(axis)
    pieces = [rows]
    for step in range(1, size):
        pieces.append(lax.ppermute(rows, axis, [(j, (j - step) % size) for j in range(size)]))
    twice = jnp.stack(pieces + pieces)
    ordered = lax.dynamic_slice_in_dim(twice, size - own, size, 0)
    return ordered.reshape((size * rows.shape[0],) + rows.shape[1:])


def scatter_direct(terms, axis):
    size, own = peers(axis)
    parts = terms.reshape((size, terms.shape[0] // size) + terms.shape[1:])
    total = lax.dynamic_index_in_dim(parts, own, 0, keepdims=False).astype(jnp.float32)
    received = []
    for step in range(1, size):
        part = lax.dynamic_index_in_dim(parts, (own + step) % size, 0, keepdims=False)
        received.append(lax.ppermute(part, axis, [(j, (j + step) % size) for j in range(size)]))
    for part in received:
        total = total + part.astype(jnp.float32)
    return total


def sum_direct(term, axis):
    size, _ = peers(axis)
    sent = term.astype(jnp.bfloat16)
    received = [
        lax.ppermute(sent, axis, [(j, (j + step) % size) for j in range(size)])
        for step in range(1, size)
    ]
    total = term
    for part in received:
        total = total + part.astype(jnp.float32)
    return total


def finish_split(partial_out, wide_rows):
    summed = scatter_direct(partial_out.astype(jnp.bfloat16), "tp")
    own_rows = lax.dynamic_slice_in_dim(
        wide_rows, lax.axis_index("tp") * summed.shape[0], summed.shape[0], 0
    )
    return (own_rows + summed).astype(jnp.bfloat16)


def body(
    tokens,
    norm_gain,
    w_query,
    w_key,
    w_value,
    w_outgate,
    w_gates,
    gate_bias,
    w_out,
    memory,
    normalizer,
    stabilizer,
):
    heads_here = w_query.shape[2] // HEAD_SIZE
    all_heads = w_gates.shape[2] // 2
    head_first = lax.axis_index("tp") * heads_here
    current = tokens
    gathered = None
    memories = []
    normalizers = []
    maxima = []
    for layer_index in range(2):
        if gathered is None:
            gathered = gather_direct(current, "tp")
        wide_rows = gathered.astype(jnp.float32)
        square_part = jnp.sum(wide_rows * wide_rows, axis=1)
        scaled = (wide_rows * norm_gain[layer_index].astype(jnp.float32)[None, :]).astype(
            jnp.bfloat16
        )
        gate_weight = w_gates[layer_index]
        own_gates = jnp.concatenate(
            [
                lax.dynamic_slice_in_dim(gate_weight, head_first, heads_here, 1),
                lax.dynamic_slice_in_dim(gate_weight, all_heads + head_first, heads_here, 1),
            ],
            axis=1,
        )
        term_query = jnp.dot(scaled, w_query[layer_index], preferred_element_type=jnp.float32)
        term_key = jnp.dot(scaled, w_key[layer_index], preferred_element_type=jnp.float32)
        term_value = jnp.dot(scaled, w_value[layer_index], preferred_element_type=jnp.float32)
        term_outgate = jnp.dot(scaled, w_outgate[layer_index], preferred_element_type=jnp.float32)
        term_gates = jnp.dot(scaled, own_gates, preferred_element_type=jnp.float32)
        width = term_query.shape[1]
        own = scatter_direct(
            jnp.concatenate(
                [term_query, term_key, term_value, term_outgate, term_gates, square_part[:, None]],
                axis=1,
            ),
            "dp",
        )
        sum_query = own[:, :width]
        sum_key = own[:, width : 2 * width]
        sum_value = own[:, 2 * width : 3 * width]
        sum_outgate = own[:, 3 * width : 4 * width]
        sum_gates = own[:, 4 * width : 4 * width + 2 * heads_here]
        square_own = own[:, 4 * width + 2 * heads_here]
        inv_scale = lax.rsqrt(square_own / D + epsilon)[:, None]
        query = (sum_query * inv_scale).astype(jnp.bfloat16)
        key_rows = (sum_key * inv_scale).astype(jnp.bfloat16)
        value_rows = (sum_value * inv_scale).astype(jnp.bfloat16)
        outgate = (sum_outgate * inv_scale).astype(jnp.bfloat16)
        gate_pre = sum_gates * inv_scale
        bias_here = gate_bias[layer_index]
        input_pre = gate_pre[:, :heads_here] + bias_here[0][None, :]
        forget_pre = gate_pre[:, heads_here:] + bias_here[1][None, :]
        readout, new_memory, new_normalizer, new_max = cell_update(
            query,
            key_rows,
            value_rows,
            input_pre,
            forget_pre,
            memory[layer_index],
            normalizer[layer_index],
            stabilizer[layer_index],
        )
        gated = (jax.nn.sigmoid(outgate.astype(jnp.float32)) * readout).astype(jnp.bfloat16)
        out_weight = w_out[layer_index]
        partial_out = jnp.dot(
            gather_direct(gated, "dp"),
            out_weight,
            preferred_element_type=jnp.float32,
        )
        if layer_index == 0:
            summed = sum_direct(partial_out, "tp")
            gathered = (wide_rows + summed).astype(jnp.bfloat16)
        else:
            current = finish_split(partial_out, wide_rows)
        memories.append(new_memory)
        normalizers.append(new_normalizer)
        maxima.append(new_max)
    return (current, jnp.stack(memories), jnp.stack(normalizers), jnp.stack(maxima))


def solution(mesh):
    placed = (
        P("tp", "dp"),
        P(None, "dp"),
        P(None, "dp", "tp"),
        P(None, "dp", "tp"),
        P(None, "dp", "tp"),
        P(None, "dp", "tp"),
        P(None, "dp", None),
        P(None, None, "tp"),
        P(None, "tp", "dp"),
        P(None, "dp", "tp", None, None),
        P(None, "dp", "tp", None),
        P(None, "dp", "tp"),
    )
    return jax.shard_map(
        body,
        mesh=mesh,
        in_specs=placed,
        out_specs=(
            P("tp", "dp"),
            P(None, "dp", "tp", None, None),
            P(None, "dp", "tp", None),
            P(None, "dp", "tp"),
        ),
        check_vma=False,
    )
```

```python
import jax
import jax.numpy as jnp
from jax import lax
from jax.sharding import PartitionSpec as P

D = 4096
HEAD_SIZE = 128


epsilon = 1e-06


def cell_update(query, key_rows, value_rows, input_pre, forget_pre, memory, normalizer, stabilizer):
    batch_size = query.shape[0]
    head_count = input_pre.shape[1]
    query_float = query.astype(jnp.float32).reshape(batch_size, head_count, -1)
    key_float = key_rows.astype(jnp.float32).reshape(
        batch_size, head_count, -1
    ) * query_float.shape[2] ** (-0.5)
    value_float = value_rows.astype(jnp.float32).reshape(batch_size, head_count, -1)
    carried = jax.nn.log_sigmoid(forget_pre) + stabilizer
    new_max = jnp.maximum(carried, input_pre)
    keep_factor = jnp.exp(carried - new_max)
    write_factor = jnp.exp(input_pre - new_max)
    new_memory = (
        keep_factor[:, :, None, None] * memory
        + write_factor[:, :, None, None] * value_float[:, :, :, None] * key_float[:, :, None, :]
    )
    new_normalizer = keep_factor[:, :, None] * normalizer + write_factor[:, :, None] * key_float
    numerator = jnp.sum(new_memory * query_float[:, :, None, :], axis=3)
    denominator = jnp.sum(new_normalizer * query_float, axis=2)
    floor_value = jnp.maximum(jnp.abs(denominator), jnp.exp(-new_max))
    readout = numerator / jnp.maximum(floor_value, 1.0)[:, :, None]
    return (readout.reshape(batch_size, -1), new_memory, new_normalizer, new_max)


def peers(axis):
    size = lax.axis_size(axis)
    return size, lax.axis_index(axis)


def gather_direct(rows, axis):
    size, own = peers(axis)
    pieces = [rows]
    for step in range(1, size):
        pieces.append(lax.ppermute(rows, axis, [(j, (j - step) % size) for j in range(size)]))
    twice = jnp.stack(pieces + pieces)
    ordered = lax.dynamic_slice_in_dim(twice, size - own, size, 0)
    return ordered.reshape((size * rows.shape[0],) + rows.shape[1:])


def scatter_direct(terms, axis):
    size, own = peers(axis)
    parts = terms.reshape((size, terms.shape[0] // size) + terms.shape[1:])
    total = lax.dynamic_index_in_dim(parts, own, 0, keepdims=False).astype(jnp.float32)
    received = []
    for step in range(1, size):
        part = lax.dynamic_index_in_dim(parts, (own + step) % size, 0, keepdims=False)
        received.append(lax.ppermute(part, axis, [(j, (j + step) % size) for j in range(size)]))
    for part in received:
        total = total + part.astype(jnp.float32)
    return total


def pairing(axis):
    size, own = peers(axis)
    inner = 2 if size % 2 == 0 else 1
    return size, inner, size // inner, own // inner, own % inner


def swap(value, axis, size):
    return lax.ppermute(value, axis, [(j, j ^ 1) for j in range(size)])


def gather_paired(rows, axis):
    size, inner, groups, group, place = pairing(axis)
    both = rows
    if inner == 2:
        other = swap(rows, axis, size)
        both = jnp.concatenate(
            [jnp.where(place == 0, rows, other), jnp.where(place == 0, other, rows)], axis=0
        )
    pieces = [both]
    for step in range(1, groups):
        hop = step * inner
        pieces.append(lax.ppermute(both, axis, [(j, (j - hop) % size) for j in range(size)]))
    twice = jnp.stack(pieces + pieces)
    ordered = lax.dynamic_slice_in_dim(twice, groups - group, groups, 0)
    return ordered.reshape((size * rows.shape[0],) + rows.shape[1:])


def sum_paired(term, axis):
    size, inner, groups, _, _ = pairing(axis)
    total = term
    if inner == 2:
        total = total + swap(term.astype(jnp.bfloat16), axis, size).astype(jnp.float32)
    sent = total.astype(jnp.bfloat16)
    received = [
        lax.ppermute(sent, axis, [(j, (j + step * inner) % size) for j in range(size)])
        for step in range(1, groups)
    ]
    for part in received:
        total = total + part.astype(jnp.float32)
    return total


def scatter_paired(term, axis):
    size, inner, groups, group, place = pairing(axis)
    parts = term.reshape((groups, inner, term.shape[0] // size) + term.shape[1:])
    half = lax.dynamic_index_in_dim(parts, place, 1, keepdims=False)
    if inner == 2:
        given = lax.dynamic_index_in_dim(parts, 1 - place, 1, keepdims=False)
        half = half + swap(given.astype(jnp.bfloat16), axis, size).astype(jnp.float32)
    total = lax.dynamic_index_in_dim(half, group, 0, keepdims=False)
    sent = half.astype(jnp.bfloat16)
    received = []
    for step in range(1, groups):
        part = lax.dynamic_index_in_dim(sent, (group + step) % groups, 0, keepdims=False)
        hop = step * inner
        received.append(lax.ppermute(part, axis, [(j, (j + hop) % size) for j in range(size)]))
    for part in received:
        total = total + part.astype(jnp.float32)
    return total


def finish_split(partial_out, wide_rows):
    summed = scatter_paired(partial_out, "tp")
    own_rows = lax.dynamic_slice_in_dim(
        wide_rows, lax.axis_index("tp") * summed.shape[0], summed.shape[0], 0
    )
    return (own_rows + summed).astype(jnp.bfloat16)


def body(
    tokens,
    norm_gain,
    w_query,
    w_key,
    w_value,
    w_outgate,
    w_gates,
    gate_bias,
    w_out,
    memory,
    normalizer,
    stabilizer,
):
    heads_here = w_query.shape[2] // HEAD_SIZE
    all_heads = w_gates.shape[2] // 2
    head_first = lax.axis_index("tp") * heads_here
    current = tokens
    gathered = None
    memories = []
    normalizers = []
    maxima = []
    for layer_index in range(2):
        if gathered is None:
            gathered = gather_paired(current, "tp")
        wide_rows = gathered.astype(jnp.float32)
        square_part = jnp.sum(wide_rows * wide_rows, axis=1)
        scaled = (wide_rows * norm_gain[layer_index].astype(jnp.float32)[None, :]).astype(
            jnp.bfloat16
        )
        gate_weight = w_gates[layer_index]
        own_gates = jnp.concatenate(
            [
                lax.dynamic_slice_in_dim(gate_weight, head_first, heads_here, 1),
                lax.dynamic_slice_in_dim(gate_weight, all_heads + head_first, heads_here, 1),
            ],
            axis=1,
        )
        term_query = jnp.dot(scaled, w_query[layer_index], preferred_element_type=jnp.float32)
        term_key = jnp.dot(scaled, w_key[layer_index], preferred_element_type=jnp.float32)
        term_value = jnp.dot(scaled, w_value[layer_index], preferred_element_type=jnp.float32)
        term_outgate = jnp.dot(scaled, w_outgate[layer_index], preferred_element_type=jnp.float32)
        term_gates = jnp.dot(scaled, own_gates, preferred_element_type=jnp.float32)
        width = term_query.shape[1]
        own = scatter_direct(
            jnp.concatenate(
                [term_query, term_key, term_value, term_outgate, term_gates, square_part[:, None]],
                axis=1,
            ),
            "dp",
        )
        sum_query = own[:, :width]
        sum_key = own[:, width : 2 * width]
        sum_value = own[:, 2 * width : 3 * width]
        sum_outgate = own[:, 3 * width : 4 * width]
        sum_gates = own[:, 4 * width : 4 * width + 2 * heads_here]
        square_own = own[:, 4 * width + 2 * heads_here]
        inv_scale = lax.rsqrt(square_own / D + epsilon)[:, None]
        query = (sum_query * inv_scale).astype(jnp.bfloat16)
        key_rows = (sum_key * inv_scale).astype(jnp.bfloat16)
        value_rows = (sum_value * inv_scale).astype(jnp.bfloat16)
        outgate = (sum_outgate * inv_scale).astype(jnp.bfloat16)
        gate_pre = sum_gates * inv_scale
        bias_here = gate_bias[layer_index]
        input_pre = gate_pre[:, :heads_here] + bias_here[0][None, :]
        forget_pre = gate_pre[:, heads_here:] + bias_here[1][None, :]
        readout, new_memory, new_normalizer, new_max = cell_update(
            query,
            key_rows,
            value_rows,
            input_pre,
            forget_pre,
            memory[layer_index],
            normalizer[layer_index],
            stabilizer[layer_index],
        )
        gated = (jax.nn.sigmoid(outgate.astype(jnp.float32)) * readout).astype(jnp.bfloat16)
        out_weight = w_out[layer_index]
        partial_out = jnp.dot(
            gather_direct(gated, "dp"),
            out_weight,
            preferred_element_type=jnp.float32,
        )
        if layer_index == 0:
            summed = sum_paired(partial_out, "tp")
            gathered = (wide_rows + summed).astype(jnp.bfloat16)
        else:
            current = finish_split(partial_out, wide_rows)
        memories.append(new_memory)
        normalizers.append(new_normalizer)
        maxima.append(new_max)
    return (current, jnp.stack(memories), jnp.stack(normalizers), jnp.stack(maxima))


def solution(mesh):
    placed = (
        P("tp", "dp"),
        P(None, "dp"),
        P(None, "dp", "tp"),
        P(None, "dp", "tp"),
        P(None, "dp", "tp"),
        P(None, "dp", "tp"),
        P(None, "dp", None),
        P(None, None, "tp"),
        P(None, "tp", "dp"),
        P(None, "dp", "tp", None, None),
        P(None, "dp", "tp", None),
        P(None, "dp", "tp"),
    )
    return jax.shard_map(
        body,
        mesh=mesh,
        in_specs=placed,
        out_specs=(
            P("tp", "dp"),
            P(None, "dp", "tp", None, None),
            P(None, "dp", "tp", None),
            P(None, "dp", "tp"),
        ),
        check_vma=False,
    )
```

```python
import jax
import jax.numpy as jnp
from jax import lax
from jax.sharding import PartitionSpec as P

D = 4096
HEAD_SIZE = 128


epsilon = 1e-06


def cell_update(query, key_rows, value_rows, input_pre, forget_pre, memory, normalizer, stabilizer):
    batch_size = query.shape[0]
    head_count = input_pre.shape[1]
    query_float = query.astype(jnp.float32).reshape(batch_size, head_count, -1)
    key_float = key_rows.astype(jnp.float32).reshape(
        batch_size, head_count, -1
    ) * query_float.shape[2] ** (-0.5)
    value_float = value_rows.astype(jnp.float32).reshape(batch_size, head_count, -1)
    carried = jax.nn.log_sigmoid(forget_pre) + stabilizer
    new_max = jnp.maximum(carried, input_pre)
    keep_factor = jnp.exp(carried - new_max)
    write_factor = jnp.exp(input_pre - new_max)
    new_memory = (
        keep_factor[:, :, None, None] * memory
        + write_factor[:, :, None, None] * value_float[:, :, :, None] * key_float[:, :, None, :]
    )
    new_normalizer = keep_factor[:, :, None] * normalizer + write_factor[:, :, None] * key_float
    numerator = jnp.sum(new_memory * query_float[:, :, None, :], axis=3)
    denominator = jnp.sum(new_normalizer * query_float, axis=2)
    floor_value = jnp.maximum(jnp.abs(denominator), jnp.exp(-new_max))
    readout = numerator / jnp.maximum(floor_value, 1.0)[:, :, None]
    return (readout.reshape(batch_size, -1), new_memory, new_normalizer, new_max)


def peers(axis):
    size = lax.axis_size(axis)
    return size, lax.axis_index(axis)


def gather_direct(rows, axis):
    size, own = peers(axis)
    pieces = [rows]
    for step in range(1, size):
        pieces.append(lax.ppermute(rows, axis, [(j, (j - step) % size) for j in range(size)]))
    twice = jnp.stack(pieces + pieces)
    ordered = lax.dynamic_slice_in_dim(twice, size - own, size, 0)
    return ordered.reshape((size * rows.shape[0],) + rows.shape[1:])


def scatter_direct(terms, axis):
    size, own = peers(axis)
    parts = terms.reshape((size, terms.shape[0] // size) + terms.shape[1:])
    total = lax.dynamic_index_in_dim(parts, own, 0, keepdims=False).astype(jnp.float32)
    received = []
    for step in range(1, size):
        part = lax.dynamic_index_in_dim(parts, (own + step) % size, 0, keepdims=False)
        received.append(lax.ppermute(part, axis, [(j, (j + step) % size) for j in range(size)]))
    for part in received:
        total = total + part.astype(jnp.float32)
    return total


def pairing(axis):
    size, own = peers(axis)
    inner = 2 if size % 2 == 0 else 1
    return size, inner, size // inner, own // inner, own % inner


def swap(value, axis, size):
    return lax.ppermute(value, axis, [(j, j ^ 1) for j in range(size)])


def gather_paired(rows, axis):
    size, inner, groups, group, place = pairing(axis)
    both = rows
    if inner == 2:
        other = swap(rows, axis, size)
        both = jnp.concatenate(
            [jnp.where(place == 0, rows, other), jnp.where(place == 0, other, rows)], axis=0
        )
    pieces = [both]
    for step in range(1, groups):
        hop = step * inner
        pieces.append(lax.ppermute(both, axis, [(j, (j - hop) % size) for j in range(size)]))
    twice = jnp.stack(pieces + pieces)
    ordered = lax.dynamic_slice_in_dim(twice, groups - group, groups, 0)
    return ordered.reshape((size * rows.shape[0],) + rows.shape[1:])


def sum_paired(term, axis):
    size = lax.axis_size(axis)
    if size & (size - 1):
        return lax.psum(term, axis)
    total = term
    for mask in [1] + [2 * (2 << bit) - 2 for bit in range(size.bit_length() - 2)]:
        sent = total.astype(jnp.bfloat16)
        part = lax.ppermute(sent, axis, [(j, j ^ mask) for j in range(size)])
        total = total + part.astype(jnp.float32)
    return total


def scatter_paired(term, axis):
    size, inner, groups, group, place = pairing(axis)
    parts = term.reshape((groups, inner, term.shape[0] // size) + term.shape[1:])
    half = lax.dynamic_index_in_dim(parts, place, 1, keepdims=False)
    if inner == 2:
        given = lax.dynamic_index_in_dim(parts, 1 - place, 1, keepdims=False)
        half = half + swap(given.astype(jnp.bfloat16), axis, size).astype(jnp.float32)
    total = lax.dynamic_index_in_dim(half, group, 0, keepdims=False)
    sent = half.astype(jnp.bfloat16)
    received = []
    for step in range(1, groups):
        part = lax.dynamic_index_in_dim(sent, (group + step) % groups, 0, keepdims=False)
        hop = step * inner
        received.append(lax.ppermute(part, axis, [(j, (j + hop) % size) for j in range(size)]))
    for part in received:
        total = total + part.astype(jnp.float32)
    return total


def finish_split(partial_out, wide_rows):
    summed = scatter_paired(partial_out, "tp")
    own_rows = lax.dynamic_slice_in_dim(
        wide_rows, lax.axis_index("tp") * summed.shape[0], summed.shape[0], 0
    )
    return (own_rows + summed).astype(jnp.bfloat16)


def body(
    tokens,
    norm_gain,
    w_query,
    w_key,
    w_value,
    w_outgate,
    w_gates,
    gate_bias,
    w_out,
    memory,
    normalizer,
    stabilizer,
):
    heads_here = w_query.shape[2] // HEAD_SIZE
    all_heads = w_gates.shape[2] // 2
    head_first = lax.axis_index("tp") * heads_here
    current = tokens
    gathered = None
    memories = []
    normalizers = []
    maxima = []
    for layer_index in range(2):
        if gathered is None:
            gathered = gather_paired(current, "tp")
        wide_rows = gathered.astype(jnp.float32)
        square_part = jnp.sum(wide_rows * wide_rows, axis=1)
        scaled = (wide_rows * norm_gain[layer_index].astype(jnp.float32)[None, :]).astype(
            jnp.bfloat16
        )
        gate_weight = w_gates[layer_index]
        own_gates = jnp.concatenate(
            [
                lax.dynamic_slice_in_dim(gate_weight, head_first, heads_here, 1),
                lax.dynamic_slice_in_dim(gate_weight, all_heads + head_first, heads_here, 1),
            ],
            axis=1,
        )
        term_query = jnp.dot(scaled, w_query[layer_index], preferred_element_type=jnp.float32)
        term_key = jnp.dot(scaled, w_key[layer_index], preferred_element_type=jnp.float32)
        term_value = jnp.dot(scaled, w_value[layer_index], preferred_element_type=jnp.float32)
        term_outgate = jnp.dot(scaled, w_outgate[layer_index], preferred_element_type=jnp.float32)
        term_gates = jnp.dot(scaled, own_gates, preferred_element_type=jnp.float32)
        width = term_query.shape[1]
        own = scatter_direct(
            jnp.concatenate(
                [term_query, term_key, term_value, term_outgate, term_gates, square_part[:, None]],
                axis=1,
            ),
            "dp",
        )
        sum_query = own[:, :width]
        sum_key = own[:, width : 2 * width]
        sum_value = own[:, 2 * width : 3 * width]
        sum_outgate = own[:, 3 * width : 4 * width]
        sum_gates = own[:, 4 * width : 4 * width + 2 * heads_here]
        square_own = own[:, 4 * width + 2 * heads_here]
        inv_scale = lax.rsqrt(square_own / D + epsilon)[:, None]
        query = (sum_query * inv_scale).astype(jnp.bfloat16)
        key_rows = (sum_key * inv_scale).astype(jnp.bfloat16)
        value_rows = (sum_value * inv_scale).astype(jnp.bfloat16)
        outgate = (sum_outgate * inv_scale).astype(jnp.bfloat16)
        gate_pre = sum_gates * inv_scale
        bias_here = gate_bias[layer_index]
        input_pre = gate_pre[:, :heads_here] + bias_here[0][None, :]
        forget_pre = gate_pre[:, heads_here:] + bias_here[1][None, :]
        readout, new_memory, new_normalizer, new_max = cell_update(
            query,
            key_rows,
            value_rows,
            input_pre,
            forget_pre,
            memory[layer_index],
            normalizer[layer_index],
            stabilizer[layer_index],
        )
        gated = (jax.nn.sigmoid(outgate.astype(jnp.float32)) * readout).astype(jnp.bfloat16)
        out_weight = w_out[layer_index]
        partial_out = jnp.dot(
            gather_direct(gated, "dp"),
            out_weight,
            preferred_element_type=jnp.float32,
        )
        if layer_index == 0:
            summed = sum_paired(partial_out, "tp")
            gathered = (wide_rows + summed).astype(jnp.bfloat16)
        else:
            current = finish_split(partial_out, wide_rows)
        memories.append(new_memory)
        normalizers.append(new_normalizer)
        maxima.append(new_max)
    return (current, jnp.stack(memories), jnp.stack(normalizers), jnp.stack(maxima))


def solution(mesh):
    placed = (
        P("tp", "dp"),
        P(None, "dp"),
        P(None, "dp", "tp"),
        P(None, "dp", "tp"),
        P(None, "dp", "tp"),
        P(None, "dp", "tp"),
        P(None, "dp", None),
        P(None, None, "tp"),
        P(None, "tp", "dp"),
        P(None, "dp", "tp", None, None),
        P(None, "dp", "tp", None),
        P(None, "dp", "tp"),
    )
    return jax.shard_map(
        body,
        mesh=mesh,
        in_specs=placed,
        out_specs=(
            P("tp", "dp"),
            P(None, "dp", "tp", None, None),
            P(None, "dp", "tp", None),
            P(None, "dp", "tp"),
        ),
        check_vma=False,
    )
```
